32 devices in a mesh: grp: 2 (over y), ep: 8 (over z, x), tp: 2 (over core).
Axes of the slice: x: 2, y: 2, z: 4, core: 2. Of those that a mesh axis runs over, the one named last changes fastest.
Arguments:
- tokens: bfloat16 [1024, 2048], P(('grp', 'ep')), parts along dimension 0, may hold values from -6 to 6
- chosen: int32 [1, 16, 9], P(None, ('grp', 'ep')), parts along dimension 1, may hold values from -1 to 63, as said below
- route_weight: float32 [1, 16, 9], P(None, ('grp', 'ep')), parts along dimension 1, may hold values from 0.1 to 1
- expert_gate: bfloat16 [2048, 4096], P(None, ('ep', 'tp')), may hold values from -0.125 to 0.125
- expert_up: bfloat16 [2048, 4096], P(None, ('ep', 'tp')), may hold values from -0.125 to 0.125
- expert_down: bfloat16 [4096, 2048], P(('ep', 'tp')), may hold values from -0.09375 to 0.09375
- dense_gate: bfloat16 [2048, 512], P('ep', 'tp'), may hold values from -0.125 to 0.125
- dense_up: bfloat16 [2048, 512], P('ep', 'tp'), may hold values from -0.125 to 0.125
- dense_down: bfloat16 [512, 2048], P('tp', 'ep'), may hold values from -0.25 to 0.25
- branch_gate: float32 [2048], P('tp'), may hold values from -6 to 6
Outputs:
- mixed: bfloat16 [1024, 2048], P(('grp', 'ep'), 'tp'), parts along dimension 0
The draws below stay inside these ranges and needn't reach their ends.
There are 2 independent parts, one for each index of `grp`. The reference program is written for one: setup_inputs(seed, part) draws one part's arguments, and reference() takes and returns one part's arrays. A program takes and returns all parts, laid end to end along the dimension named above; an argument that names none is the same for every part. Nothing has to cross between parts.
Inputs may be any that keep to these rules, and one draw needn't show every extreme that they name: chosen[e, s, k] is -1 or an index local to device s (token s * 64 + chosen[e, s, k] of the whole). In each (e, s) row the live entries come first and are distinct, the -1 entries follow. Each expert takes exactly 64 tokens in all, at most 9 from one device, and for every expert some device gives it exactly 9.
All inputs are finite; a program needn't handle non-finite values.
Results may differ from the reference program's by a relative error of at most 0.0085.
Values may be sent and summed in bfloat16 or wider, within the bound.
A program may use at most 64 MiB of HBM per device.

```python
import jax
import jax.numpy as jnp
from jax import lax

D = 2048
FF = 4096
DH = 512
TOK_DEV = 64
EXPERTS = 1
SLOT = 9
TOKENS = 512
N_EP = 8


def draw_chosen(key, part):
    middle = TOK_DEV // 8
    spread = SLOT - middle
    pairs = N_EP // 2
    base = jax.random.fold_in(key, 17)
    key_shift = jax.random.fold_in(base, 1)
    key_top = jax.random.fold_in(base, 2)
    key_order = jax.random.fold_in(base, 3)
    shift = jax.random.randint(key_shift, (EXPERTS, pairs), -spread, spread + 1)
    top_pair = jax.random.randint(key_top, (EXPERTS,), 0, pairs)
    shift = jnp.where(jnp.arange(pairs)[None, :] == top_pair[:, None], spread, shift)
    counts = jnp.stack([middle + shift, middle - shift], axis=-1).reshape(EXPERTS, N_EP)
    order_keys = jax.random.split(key_order, EXPERTS * N_EP)
    orders = jax.vmap(lambda single: jax.random.permutation(single, TOK_DEV))(order_keys).reshape(EXPERTS, N_EP, TOK_DEV)
    slots_iota = jnp.arange(SLOT)
    return jnp.where(slots_iota[None, None, :] < counts[:, :, None], orders[:, :, :SLOT], -1).astype(jnp.int32)


def levels(rng, dims, cuts, least, largest):
    factor_of, own = 1.0, jax.random.fold_in(rng, 6)
    for axis_at, blocks in cuts:
        steps = jnp.exp(jax.random.uniform(jax.random.fold_in(own, axis_at), (blocks,), jnp.float32, least / len(cuts), largest / len(cuts)))
        factor_of = factor_of * jnp.repeat(steps, dims[axis_at] // blocks).reshape([-1 if axis == axis_at else 1 for axis in range(len(dims))])
    return factor_of


def normal_values(key, dims, scale, bound, shards=(), held_as=jnp.bfloat16):
    result = scale * jax.random.normal(key, dims, jnp.float32)
    if shards:
        result = result * levels(key, dims, shards, -0.22, 0.18)
    return jnp.clip(result, -bound, bound).astype(held_as)


def setup_inputs(seed: int = 0, part: int = 0) -> dict:
    key_of = jax.random.split(jax.random.key(seed), 11)
    part_keys = jax.random.split(jax.random.fold_in(key_of[10], part), 11)
    return {
        "tokens": normal_values(part_keys[0], (TOKENS, D), 1.0, 6.0, ((0, 8),)),
        "chosen": draw_chosen(jax.random.fold_in(jax.random.fold_in(key_of[10], part), 71), part),
        "route_weight": jnp.clip(0.1 + 0.9 * jax.random.uniform(part_keys[2], (EXPERTS, N_EP, SLOT), jnp.float32) ** levels(part_keys[2], (EXPERTS, N_EP, SLOT), ((1, 8),), -0.2, 0.2), 0.1, 1.0),
        "expert_gate": normal_values(key_of[3], (D, EXPERTS * FF), D ** -0.5, 0.125, ((1, 16),)),
        "expert_up": normal_values(key_of[4], (D, EXPERTS * FF), D ** -0.5, 0.125, ((1, 16),)),
        "expert_down": normal_values(key_of[5], (EXPERTS * FF, D), FF ** -0.5, 0.09375, ((0, 16),)),
        "dense_gate": normal_values(key_of[6], (D, DH), D ** -0.5, 0.125, ((0, 8), (1, 2))),
        "dense_up": normal_values(key_of[7], (D, DH), D ** -0.5, 0.125, ((0, 8), (1, 2))),
        "dense_down": normal_values(key_of[8], (DH, D), DH ** -0.5, 0.25, ((0, 2), (1, 8))),
        "branch_gate": normal_values(key_of[9], (D,), 2.0, 6.0, ((0, 2),), jnp.float32),
    }


def reference(tokens, chosen, route_weight, expert_gate, expert_up, expert_down, dense_gate, dense_up, dense_down, branch_gate):
    rows_all = N_EP * SLOT
    offsets = (jnp.arange(N_EP, dtype=jnp.int32) * TOK_DEV)[:, None]

    def one_expert(totals, expert_id):
        picked = lax.dynamic_index_in_dim(chosen, expert_id, 0, keepdims=False)
        filled = picked >= 0
        token_index = (jnp.maximum(picked, 0) + offsets).reshape(-1).astype(jnp.int32)
        token_rows = jnp.where(filled.reshape(-1)[:, None], tokens[token_index], jnp.zeros((), jnp.bfloat16))
        first = (expert_id * FF).astype(jnp.int32)
        gate_cols = lax.dynamic_slice_in_dim(expert_gate, first, FF, 1)
        up_cols = lax.dynamic_slice_in_dim(expert_up, first, FF, 1)
        gate_act = jnp.dot(token_rows, gate_cols, preferred_element_type=jnp.float32)
        up_act = jnp.dot(token_rows, up_cols, preferred_element_type=jnp.float32)
        hidden = (jax.nn.silu(gate_act) * up_act).astype(jnp.bfloat16)
        down_rows = lax.dynamic_slice_in_dim(expert_down, first, FF, 0).reshape(16, FF // 16, D)
        block_sums = jnp.einsum("rbh,bhd->brd", hidden.reshape(rows_all, 16, FF // 16).astype(jnp.float32), down_rows.astype(jnp.float32)).astype(jnp.bfloat16)
        block_sums = lax.optimization_barrier(block_sums)
        members = block_sums.astype(jnp.float32).reshape(8, 2, rows_all, D).sum(axis=1).astype(jnp.bfloat16)
        members = lax.optimization_barrier(members)
        expert_out = members.astype(jnp.float32).sum(axis=0)
        scale = (lax.dynamic_index_in_dim(route_weight, expert_id, 0, keepdims=False) * filled).reshape(-1)
        totals = totals.at[token_index].add(expert_out * scale[:, None])
        return totals, None

    combined, _ = lax.scan(one_expert, jnp.zeros((N_EP * TOK_DEV, D), jnp.float32), jnp.arange(EXPERTS, dtype=jnp.int32))
    gate_dense = jnp.dot(tokens, dense_gate, preferred_element_type=jnp.float32)
    up_dense = jnp.dot(tokens, dense_up, preferred_element_type=jnp.float32)
    dense_hidden = (jax.nn.silu(gate_dense) * up_dense).astype(jnp.bfloat16)
    half = DH // 2
    first_part = jnp.dot(dense_hidden[:, :half], dense_down[:half], preferred_element_type=jnp.float32).astype(jnp.bfloat16)
    second_part = jnp.dot(dense_hidden[:, half:], dense_down[half:], preferred_element_type=jnp.float32).astype(jnp.bfloat16)
    first_part, second_part = lax.optimization_barrier((first_part, second_part))
    dense_sum = first_part.astype(jnp.float32) + second_part.astype(jnp.float32)
    return (combined + jax.nn.sigmoid(branch_gate)[None, :] * dense_sum).astype(jnp.bfloat16)
```

```python
import functools

import jax
import jax.numpy as jnp
from jax import lax
from jax.experimental import pallas as pl
from jax.experimental.pallas import tpu as pltpu
from jax.sharding import PartitionSpec as P

MESH = pl.DeviceIdType.MESH


def swapped(block, axis, apart):
    count = lax.axis_size(axis)
    route = []
    for low in range(count):
        high = low | 1 << apart
        if high != low and high < count:
            route += [(low, high), (high, low)]
    return lax.ppermute(block, axis, route)


def expert_hidden(received, gate_cols, up_cols):
    flat_rows = received.reshape(-1, received.shape[-1])
    gate_act = jnp.dot(flat_rows, gate_cols, preferred_element_type=jnp.float32)
    up_act = jnp.dot(flat_rows, up_cols, preferred_element_type=jnp.float32)
    hidden = (jax.nn.silu(gate_act) * up_act).astype(jnp.bfloat16)
    return hidden.reshape(received.shape[0], received.shape[1], gate_cols.shape[1])


def join_pieces(mine, theirs, upper):
    return jnp.where(upper, jnp.concatenate([theirs, mine], 2), jnp.concatenate([mine, theirs], 2))


def fused_kernel(
    n,
    tok_ref,
    chosen_ref,
    route_ref,
    eg_hbm,
    eu_hbm,
    ed_hbm,
    dg_ref,
    du_ref,
    dd_ref,
    bg_ref,
    out_ref,
    eg,
    eu,
    ed,
    weights,
    tok_all,
    table,
    rows_all,
    part_send,
    part_recv,
    hid_all,
    down_send,
    down_recv,
    half_send,
    half_recv,
    ret_send,
    ret_recv,
    local_sem,
    w_send,
    w_recv,
    t_send,
    t_recv,
    tf_send,
    tf_recv,
    r_send,
    r_recv,
    rf_send,
    rf_recv,
    p_send,
    p_recv,
    h_send,
    h_recv,
    d_send,
    d_recv,
    s_send,
    s_recv,
    m_send,
    m_recv,
):
    f32, bf16 = jnp.float32, jnp.bfloat16
    ep, tp = lax.axis_index("ep"), lax.axis_index("tp")
    sib = 1 - tp
    nz = n // 2
    x, z = lax.rem(ep, 2), lax.div(ep, 2)
    toks, width = tok_ref.shape
    feat = width // nz
    halfw = width // 2
    spad = rows_all.shape[2]
    hidden = dg_ref.shape[1]
    pos_count = nz // 2

    def line(d):
        return lax.rem(z + d + nz, nz) * 2 + x

    def ring(d):
        return lax.rem(ep + d + n, n)

    sends = []

    def remote(src, dst, ssem, rsem, to_ep, to_tp, go=True):
        copy = pltpu.make_async_remote_copy(
            src_ref=src,
            dst_ref=dst,
            send_sem=ssem,
            recv_sem=rsem,
            device_id={"ep": to_ep, "tp": to_tp},
            device_id_type=MESH,
        )
        if go:
            copy.start()
            sends.append(copy)
        return copy

    loads = []
    for i, (src, dst) in enumerate(((eg_hbm, eg), (eu_hbm, eu), (ed_hbm, ed))):
        load = pltpu.make_async_copy(src, dst, local_sem.at[i])
        load.start()
        loads.append(load)

    barrier = pltpu.get_barrier_semaphore()
    for d in range(1, n):
        pl.semaphore_signal(
            barrier, inc=1, device_id={"ep": ring(d), "tp": tp}, device_id_type=MESH
        )
    for d in range(nz):
        pl.semaphore_signal(
            barrier, inc=1, device_id={"ep": line(d), "tp": sib}, device_id_type=MESH
        )

    table[...] = jnp.full(table.shape, -1.0, f32)
    slots = chosen_ref.shape[2]
    table[0:1, 0:slots] = chosen_ref[0].astype(f32)
    table[8:9, 0:slots] = route_ref[0]
    token_id = lax.broadcasted_iota(jnp.int32, (toks, table.shape[1]), 0).astype(f32)
    match = token_id == table[0:1, :]
    onehot = jnp.where(match, 1.0, 0.0).astype(f32)
    pick = onehot.T[:spad].astype(bf16)
    picked = jnp.dot(pick, tok_ref[...], preferred_element_type=f32).astype(bf16)
    rows_all[0, 0] = picked[:, :halfw]
    rows_all[1, 0] = picked[:, halfw:]

    pl.semaphore_wait(barrier, n - 1 + nz)

    th = toks // 2
    mine = pl.ds(pl.multiple_of(tp * th, th), th)
    theirs = pl.ds(pl.multiple_of(sib * th, th), th)
    tcopies = []
    for d in range(1, nz):
        cols = pl.ds(pl.multiple_of(lax.rem(z + d, nz) * feat, feat), feat)
        tcopies.append(
            remote(
                tok_ref.at[mine, cols],
                tok_all.at[d, mine],
                t_send.at[d],
                t_recv.at[d],
                line(d),
                tp,
            )
        )
    pair = ep + 1 - 2 * x
    wcopies = []
    for i, src in enumerate((dg_ref, du_ref, dd_ref)):
        wcopies.append(
            remote(src, weights.at[i, x], w_send.at[i], w_recv.at[i], pair, tp)
        )
    rcopies = []
    for d in range(1, n):
        rcopies.append(
            remote(
                rows_all.at[tp, 0], rows_all.at[tp, d], r_send.at[d], r_recv.at[d], ring(d), tp
            )
        )

    own_cols = pl.ds(pl.multiple_of(z * feat, feat), feat)
    tok_all[0] = tok_ref[:, own_cols]
    for i, src in enumerate((dg_ref, du_ref, dd_ref)):
        weights[i, x] = src[...]

    for d in range(1, nz):
        tcopies[d - 1].wait_recv()
        remote(
            tok_all.at[d, mine], tok_all.at[d, mine], tf_send.at[d], tf_recv.at[d], ep, sib
        )
    wait_at = lambda dst, ssem, rsem: remote(dst, dst, ssem, rsem, ep, sib, go=False).wait_recv()

    def wait_on(ssem, rsem, dst):
        wait_at(dst, ssem, rsem)

    for i in range(2):
        remote(dg_ref, weights.at[i, 1 - x], w_send.at[i], w_recv.at[i], pair, tp, go=False).wait_recv()
    for d in range(1, nz):
        wait_on(tf_send.at[d], tf_recv.at[d], tok_all.at[d, theirs])
    toks_in = tok_all[...].reshape(nz * toks, feat)
    fh = feat // 2
    sums = []
    for i in range(2):
        total = jnp.dot(toks_in[:, :fh], weights[i, 0], preferred_element_type=f32) + jnp.dot(
            toks_in[:, fh:], weights[i, 1], preferred_element_type=f32
        )
        sums.append(total[:toks])
        for d in range(1, nz):
            part_send[d - 1, i] = total[d * toks : (d + 1) * toks].astype(bf16)
    pcopies = []
    for d in range(1, nz):
        pcopies.append(
            remote(
                part_send.at[d - 1], part_recv.at[d - 1], p_send.at[d], p_recv.at[d], line(-d), tp
            )
        )

    for d in range(1, n):
        rcopies[d - 1].wait_recv()
        remote(
            rows_all.at[tp, d], rows_all.at[tp, d], rf_send.at[d], rf_recv.at[d], ep, sib
        )
    for load in loads[:2]:
        load.wait()
    for d in range(1, n):
        wait_on(rf_send.at[d], rf_recv.at[d], rows_all.at[sib, d])
    low = rows_all[0].reshape(n * spad, halfw)
    high = rows_all[1].reshape(n * spad, halfw)

    def project(w):
        return jnp.dot(low, w[:halfw], preferred_element_type=f32) + jnp.dot(
            high, w[halfw:], preferred_element_type=f32
        )

    gate = project(eg)
    up = project(eu)
    act = (gate / (1.0 + jnp.exp(-gate)) * up).astype(bf16)
    loads[2].wait()
    off = pl.ds(pl.multiple_of(sib * halfw, halfw), halfw)
    keep = pl.ds(pl.multiple_of(tp * halfw, halfw), halfw)
    half_send[...] = jnp.dot(act, ed[:, off], preferred_element_type=f32).astype(bf16)
    scopy = remote(half_send, half_recv, s_send, s_recv, ep, sib)

    for d in range(1, nz):
        pcopies[d - 1].wait_recv()
        sums = [sums[i] + part_recv[d - 1, i].astype(f32) for i in range(2)]
    dense_hidden = (sums[0] / (1.0 + jnp.exp(-sums[0])) * sums[1]).astype(bf16)
    hid_all[0] = dense_hidden
    hcopies = []
    for d in range(1, nz):
        hcopies.append(
            remote(hid_all.at[0], hid_all.at[d], h_send.at[d], h_recv.at[d], line(d), tp)
        )

    own_half = jnp.dot(act, ed[:, keep], preferred_element_type=f32).astype(bf16)
    scopy.wait_recv()
    member = (own_half.astype(f32) + half_recv[...].astype(f32)).astype(bf16)
    ret_send[...] = member.reshape(n, spad, halfw)
    mcopies = []
    for d in range(1, n):
        mcopies.append(
            remote(ret_send.at[d], ret_recv.at[d - 1], m_send.at[d], m_recv.at[d], ring(-d), tp)
        )

    remote(dd_ref, weights.at[2, 1 - x], w_send.at[2], w_recv.at[2], pair, tp, go=False).wait_recv()
    for d in range(1, nz):
        hcopies[d - 1].wait_recv()
    owner = lax.div(z, pos_count)
    place = lax.rem(z, pos_count)
    hid_in = hid_all[...].reshape(nz * toks, hidden)
    for i in range(2):
        part = jnp.dot(hid_in, weights[2, i], preferred_element_type=f32).astype(bf16)
        down_send[:, :, i * fh : (i + 1) * fh] = part.reshape(nz, toks, fh)
    for d in range(1, nz):
        remote(
            down_send.at[d],
            down_recv.at[place, tp],
            d_send.at[d],
            d_recv.at[place, tp],
            line(-d),
            owner,
        )

    def sibling_copy():
        return remote(
            down_send.at[0],
            down_recv.at[place, tp],
            d_send.at[0],
            d_recv.at[place, tp],
            ep,
            sib,
            go=False,
        )

    @pl.when(owner != tp)
    def _():
        sibling_copy().start()

    @pl.when(owner == tp)
    def _():
        down_recv[place, tp] = down_send[0]

    total = ret_send[0].astype(f32)
    for d in range(1, n):
        mcopies[d - 1].wait_recv()
        total = total + ret_recv[d - 1].astype(f32)
    spread = jnp.where(match, table[8:9, :], 0.0)[:, :spad]
    combined = jnp.dot(
        spread, total, preferred_element_type=f32, precision=lax.Precision.HIGHEST
    )
    for p in range(pos_count):
        for t in range(2):

            @pl.when(jnp.logical_or(tp * pos_count + p != z, tp != t))
            def _():
                wait_on(d_send.at[0], d_recv.at[p, t], down_recv.at[p, t])

        cols = slice(p * feat, (p + 1) * feat)
        dense = down_recv[p, 0].astype(f32) + down_recv[p, 1].astype(f32)
        scale = 1.0 / (1.0 + jnp.exp(-bg_ref[:, cols]))
        out_ref[:, cols] = (combined[:, cols] + scale * dense).astype(bf16)

    for copy in sends:
        copy.wait_send()

    @pl.when(owner != tp)
    def _():
        sibling_copy().wait_send()


def fused_local(n, *args):
    tokens, chosen, dense_gate, branch_gate = args[0], args[1], args[6], args[9]
    toks, width = tokens.shape
    nz = n // 2
    feat = width // nz
    spad = -(-chosen.shape[2] // 16) * 16
    hid = dense_gate.shape[1]
    units = args[3].shape[1]
    bf16 = jnp.bfloat16
    vmem = pl.BlockSpec(memory_space=pltpu.VMEM)
    hbm = pl.BlockSpec(memory_space=pl.ANY)
    dma = pltpu.SemaphoreType.DMA
    scratch = [
        pltpu.VMEM((width, units), bf16),
        pltpu.VMEM((width, units), bf16),
        pltpu.VMEM((units, width), bf16),
        pltpu.VMEM((3, 2) + dense_gate.shape, bf16),
        pltpu.VMEM((nz, toks, feat), bf16),
        pltpu.VMEM((16, 128), jnp.float32),
        pltpu.VMEM((2, n, spad, width // 2), bf16),
        pltpu.VMEM((nz - 1, 2, toks, hid), bf16),
        pltpu.VMEM((nz - 1, 2, toks, hid), bf16),
        pltpu.VMEM((nz, toks, hid), bf16),
        pltpu.VMEM((nz, toks, feat), bf16),
        pltpu.VMEM((nz // 2, 2, toks, feat), bf16),
        pltpu.VMEM((n * spad, width // 2), bf16),
        pltpu.VMEM((n * spad, width // 2), bf16),
        pltpu.VMEM((n, spad, width // 2), bf16),
        pltpu.VMEM((n - 1, spad, width // 2), bf16),
        dma((3,)),
        dma((3,)),
        dma((3,)),
        dma((nz,)),
        dma((nz,)),
        dma((nz,)),
        dma((nz,)),
        dma((n,)),
        dma((n,)),
        dma((n,)),
        dma((n,)),
        dma((nz,)),
        dma((nz,)),
        dma((nz,)),
        dma((nz,)),
        dma((nz,)),
        dma((nz // 2, 2)),
        dma,
        dma,
        dma((n,)),
        dma((n,)),
    ]
    return pl.pallas_call(
        functools.partial(fused_kernel, n),
        out_shape=jax.ShapeDtypeStruct((toks, width // 2), bf16),
        in_specs=[vmem] * 3 + [hbm] * 3 + [vmem] * 4,
        out_specs=vmem,
        scratch_shapes=scratch,
        compiler_params=pltpu.CompilerParams(collective_id=0, has_side_effects=True),
    )(*args[:9], branch_gate.reshape(1, -1))


def local(*args):
    n = lax.axis_size("ep")
    tokens, chosen, dense_gate = args[0], args[1], args[6]
    width = tokens.shape[1]
    square = dense_gate.shape[0] == dense_gate.shape[1] == args[8].shape[1]
    fits = chosen.shape[0] == 1 and n % 4 == 0 and square
    fits = fits and (width // n) % 128 == 0 and tokens.shape[0] % 32 == 0
    fits = fits and chosen.shape[2] <= 128 and lax.axis_size("tp") == 2
    return fused_local(n, *args) if fits else plain_local(*args)


def plain_local(
    tokens,
    chosen,
    route_weight,
    expert_gate,
    expert_up,
    expert_down,
    dense_gate,
    dense_up,
    dense_down,
    branch_gate,
):
    ep_count = lax.axis_size("ep")
    experts = chosen.shape[0]
    slots = chosen.shape[2]
    tok_local = tokens.shape[0]
    width = tokens.shape[1]
    picked = chosen[:, 0, :]
    filled = picked >= 0
    token_rows = jnp.take(tokens, jnp.maximum(picked, 0).reshape(-1), axis=0).reshape(
        experts, slots, width
    )
    token_rows = jnp.where(filled[:, :, None], token_rows, jnp.zeros((), jnp.bfloat16))
    send_width = token_rows.shape[2]
    piece = send_width // 8
    split_rows = jnp.transpose(token_rows.reshape(experts, slots, 8, piece), (0, 2, 1, 3)).reshape(
        ep_count, slots, piece
    )
    own_piece = lax.all_to_all(split_rows, "ep", split_axis=0, concat_axis=0, tiled=True)
    member = lax.axis_index("ep") % 8
    current = own_piece[:, :, None, :]
    partner = swapped(current, "ep", 0)
    current = join_pieces(current, partner, member % 2 == 1)
    partner = swapped(current, "ep", 1)
    current = join_pieces(current, partner, member // 2 % 2 == 1)
    partner = swapped(current, "ep", 2)
    current = join_pieces(current, partner, member // 4 == 1)
    received = current.reshape(ep_count, slots, send_width)
    hidden = expert_hidden(received, gate_cols=expert_gate, up_cols=expert_up)
    flat_hidden = hidden.reshape(ep_count * slots, -1)
    shard_rows = expert_down
    member_sums = lax.psum_scatter(
        lax.dot_general(
            shard_rows, flat_hidden, (((0,), (1,)), ((), ())), preferred_element_type=jnp.float32
        ).astype(jnp.bfloat16),
        "tp",
        scatter_dimension=0,
        tiled=True,
    )
    returned = lax.all_to_all(member_sums, "ep", split_axis=1, concat_axis=1, tiled=True)
    summed = returned.astype(jnp.float32).reshape(width // 2, experts, 8, slots).sum(axis=2)
    positions = lax.broadcasted_iota(jnp.int32, (experts, slots, tok_local), 2)
    weights_table = jnp.where(picked[:, :, None] == positions, route_weight[:, 0, :, None], 0.0)
    combined = jnp.einsum("fek,ekt->tf", summed, weights_table, precision=lax.Precision.HIGHEST)
    shard_rows = (
        lax.all_gather(dense_gate, "ep", axis=0, tiled=True),
        lax.all_gather(dense_up, "ep", axis=0, tiled=True),
    )
    gate_dense = jnp.dot(tokens, shard_rows[0], preferred_element_type=jnp.float32)
    up_dense = jnp.dot(tokens, shard_rows[1], preferred_element_type=jnp.float32)
    dense_hidden = (jax.nn.silu(gate_dense) * up_dense).astype(jnp.bfloat16)
    dense_terms = jnp.dot(
        dense_hidden,
        lax.all_gather(dense_down, "ep", axis=1, tiled=True),
        preferred_element_type=jnp.float32,
    )
    dense_sum = lax.psum_scatter(
        dense_terms.astype(jnp.bfloat16), "tp", scatter_dimension=1, tiled=True
    ).astype(jnp.float32)
    return (combined + jax.nn.sigmoid(branch_gate)[None, :] * dense_sum).astype(jnp.bfloat16)


def solution(mesh):
    return jax.shard_map(
        local,
        mesh=mesh,
        in_specs=(
            P(("grp", "ep"), None),
            P(None, ("grp", "ep"), None),
            P(None, ("grp", "ep"), None),
            P(None, ("ep", "tp")),
            P(None, ("ep", "tp")),
            P(("ep", "tp"), None),
            P("ep", "tp"),
            P("ep", "tp"),
            P("tp", "ep"),
            P("tp"),
        ),
        out_specs=P(("grp", "ep"), "tp"),
        check_vma=False,
    )
```

```python
import functools

import jax
import jax.numpy as jnp
from jax import lax
from jax.experimental import pallas as pl
from jax.experimental.pallas import tpu as pltpu
from jax.sharding import PartitionSpec as P

MESH = pl.DeviceIdType.MESH


def swapped(block, axis, apart):
    count = lax.axis_size(axis)
    route = []
    for low in range(count):
        high = low | 1 << apart
        if high != low and high < count:
            route += [(low, high), (high, low)]
    return lax.ppermute(block, axis, route)


def expert_hidden(received, gate_cols, up_cols):
    flat_rows = received.reshape(-1, received.shape[-1])
    gate_act = jnp.dot(flat_rows, gate_cols, preferred_element_type=jnp.float32)
    up_act = jnp.dot(flat_rows, up_cols, preferred_element_type=jnp.float32)
    hidden = (jax.nn.silu(gate_act) * up_act).astype(jnp.bfloat16)
    return hidden.reshape(received.shape[0], received.shape[1], gate_cols.shape[1])


def join_pieces(mine, theirs, upper):
    return jnp.where(upper, jnp.concatenate([theirs, mine], 2), jnp.concatenate([mine, theirs], 2))


def fused_kernel(
    n,
    tok_ref,
    chosen_ref,
    route_ref,
    eg_hbm,
    eu_hbm,
    ed_hbm,
    dg_ref,
    du_ref,
    dd_ref,
    bg_ref,
    out_ref,
    eg,
    eu,
    ed,
    weights,
    tok_all,
    table,
    rows_all,
    ext_all,
    ext_wide,
    part_send,
    part_recv,
    hid_all,
    down_send,
    down_recv,
    half_send,
    half_recv,
    ret_send,
    ret_recv,
    rex_send,
    rex_recv,
    local_sem,
    w_send,
    w_recv,
    t_send,
    t_recv,
    tf_send,
    tf_recv,
    r_send,
    r_recv,
    rf_send,
    rf_recv,
    p_send,
    p_recv,
    h_send,
    h_recv,
    d_send,
    d_recv,
    s_send,
    s_recv,
    m_send,
    m_recv,
):
    f32, bf16 = jnp.float32, jnp.bfloat16
    ep, tp = lax.axis_index("ep"), lax.axis_index("tp")
    sib = 1 - tp
    nz = n // 2
    x, z = lax.rem(ep, 2), lax.div(ep, 2)
    toks, width = tok_ref.shape
    feat = width // nz
    halfw = width // 2
    base = rows_all.shape[2]
    chunks = halfw // 128
    hidden = dg_ref.shape[1]
    pos_count = nz // 2

    def line(d):
        return lax.rem(z + d + nz, nz) * 2 + x

    def ring(d):
        return lax.rem(ep + d + n, n)

    sends = []

    def remote(src, dst, ssem, rsem, to_ep, to_tp, go=True):
        copy = pltpu.make_async_remote_copy(
            src_ref=src,
            dst_ref=dst,
            send_sem=ssem,
            recv_sem=rsem,
            device_id={"ep": to_ep, "tp": to_tp},
            device_id_type=MESH,
        )
        if go:
            copy.start()
            sends.append(copy)
        return copy

    loads = []
    for i, (src, dst) in enumerate(((eg_hbm, eg), (eu_hbm, eu), (ed_hbm, ed))):
        load = pltpu.make_async_copy(src, dst, local_sem.at[i])
        load.start()
        loads.append(load)

    barrier = pltpu.get_barrier_semaphore()
    for d in range(1, n):
        pl.semaphore_signal(
            barrier, inc=1, device_id={"ep": ring(d), "tp": tp}, device_id_type=MESH
        )
    for d in range(nz):
        pl.semaphore_signal(
            barrier, inc=1, device_id={"ep": line(d), "tp": sib}, device_id_type=MESH
        )

    table[...] = jnp.full(table.shape, -1.0, f32)
    slots = chosen_ref.shape[2]
    extra = slots - base
    spad = -(-slots // 16) * 16
    table[0:1, 0:slots] = chosen_ref[0].astype(f32)
    table[8:9, 0:slots] = route_ref[0]
    token_id = lax.broadcasted_iota(jnp.int32, (toks, table.shape[1]), 0).astype(f32)
    match = token_id == table[0:1, :]
    onehot = jnp.where(match, 1.0, 0.0).astype(f32)
    pick = onehot.T[:spad].astype(bf16)
    picked = jnp.dot(pick, tok_ref[...], preferred_element_type=f32)
    for h in range(2):
        rows_all[h, 0] = picked[:base, h * halfw : (h + 1) * halfw].astype(bf16)
        pieces = [
            picked[base + k : base + k + 1, h * halfw + c * 128 : h * halfw + (c + 1) * 128]
            for k in range(extra)
            for c in range(chunks)
        ]
        ext_all[h, 0] = jnp.concatenate(pieces, 0).astype(bf16)

    pl.semaphore_wait(barrier, n - 1 + nz)

    th = toks // 2
    mine = pl.ds(pl.multiple_of(tp * th, th), th)
    theirs = pl.ds(pl.multiple_of(sib * th, th), th)
    tcopies = []
    for d in range(1, nz):
        cols = pl.ds(pl.multiple_of(lax.rem(z + d, nz) * feat, feat), feat)
        tcopies.append(
            remote(
                tok_ref.at[mine, cols],
                tok_all.at[d, mine],
                t_send.at[d],
                t_recv.at[d],
                line(d),
                tp,
            )
        )
    pair = ep + 1 - 2 * x
    wcopies = []
    for i, src in enumerate((dg_ref, du_ref, dd_ref)):
        wcopies.append(
            remote(src, weights.at[i, x], w_send.at[i], w_recv.at[i], pair, tp)
        )
    rcopies, ecopies = [], []
    for d in range(1, n):
        rcopies.append(
            remote(
                rows_all.at[tp, 0], rows_all.at[tp, d], r_send.at[d], r_recv.at[d], ring(d), tp
            )
        )
        ecopies.append(
            remote(
                ext_all.at[tp, 0],
                ext_all.at[tp, d],
                r_send.at[n + d],
                r_recv.at[n + d],
                ring(d),
                tp,
            )
        )

    own_cols = pl.ds(pl.multiple_of(z * feat, feat), feat)
    tok_all[0] = tok_ref[:, own_cols]
    for i, src in enumerate((dg_ref, du_ref, dd_ref)):
        weights[i, x] = src[...]

    for d in range(1, nz):
        tcopies[d - 1].wait_recv()
        remote(
            tok_all.at[d, mine], tok_all.at[d, mine], tf_send.at[d], tf_recv.at[d], ep, sib
        )
    wait_at = lambda dst, ssem, rsem: remote(dst, dst, ssem, rsem, ep, sib, go=False).wait_recv()

    def wait_on(ssem, rsem, dst):
        wait_at(dst, ssem, rsem)

    for i in range(2):
        remote(dg_ref, weights.at[i, 1 - x], w_send.at[i], w_recv.at[i], pair, tp, go=False).wait_recv()
    for d in range(1, nz):
        wait_on(tf_send.at[d], tf_recv.at[d], tok_all.at[d, theirs])
    toks_in = tok_all[...].reshape(nz * toks, feat)
    fh = feat // 2
    sums = []
    for i in range(2):
        total = jnp.dot(toks_in[:, :fh], weights[i, 0], preferred_element_type=f32) + jnp.dot(
            toks_in[:, fh:], weights[i, 1], preferred_element_type=f32
        )
        sums.append(total[:toks])
        for d in range(1, nz):
            part_send[d - 1, i] = total[d * toks : (d + 1) * toks].astype(bf16)
    pcopies = []
    for d in range(1, nz):
        pcopies.append(
            remote(
                part_send.at[d - 1], part_recv.at[d - 1], p_send.at[d], p_recv.at[d], line(-d), tp
            )
        )

    for d in range(1, n):
        rcopies[d - 1].wait_recv()
        remote(
            rows_all.at[tp, d], rows_all.at[tp, d], rf_send.at[d], rf_recv.at[d], ep, sib
        )
        ecopies[d - 1].wait_recv()
        remote(
            ext_all.at[tp, d], ext_all.at[tp, d], rf_send.at[n + d], rf_recv.at[n + d], ep, sib
        )
    for load in loads[:2]:
        load.wait()
    for d in range(1, n):
        wait_on(rf_send.at[d], rf_recv.at[d], rows_all.at[sib, d])
        wait_on(rf_send.at[n + d], rf_recv.at[n + d], ext_all.at[sib, d])
    ext_wide[...] = ext_all[...].astype(f32)
    every = half_send.shape[0]

    def stacked(h):
        parts = [rows_all[h].astype(f32).reshape(n * base, halfw)]
        for k in range(extra):
            parts.append(
                jnp.concatenate([ext_wide[h, :, k * chunks + c, :] for c in range(chunks)], 1)
            )
        if every > n * slots:
            parts.append(jnp.zeros((every - n * slots, halfw), f32))
        return jnp.concatenate(parts, 0).astype(bf16)

    low, high = stacked(0), stacked(1)

    def project(w):
        return jnp.dot(low, w[:halfw], preferred_element_type=f32) + jnp.dot(
            high, w[halfw:], preferred_element_type=f32
        )

    gate = project(eg)
    up = project(eu)
    act = (gate / (1.0 + jnp.exp(-gate)) * up).astype(bf16)
    loads[2].wait()
    off = pl.ds(pl.multiple_of(sib * halfw, halfw), halfw)
    keep = pl.ds(pl.multiple_of(tp * halfw, halfw), halfw)
    half_send[...] = jnp.dot(act, ed[:, off], preferred_element_type=f32).astype(bf16)
    scopy = remote(half_send, half_recv, s_send, s_recv, ep, sib)

    for d in range(1, nz):
        pcopies[d - 1].wait_recv()
        sums = [sums[i] + part_recv[d - 1, i].astype(f32) for i in range(2)]
    dense_hidden = (sums[0] / (1.0 + jnp.exp(-sums[0])) * sums[1]).astype(bf16)
    hid_all[0] = dense_hidden
    hcopies = []
    for d in range(1, nz):
        hcopies.append(
            remote(hid_all.at[0], hid_all.at[d], h_send.at[d], h_recv.at[d], line(d), tp)
        )

    own_half = jnp.dot(act, ed[:, keep], preferred_element_type=f32).astype(bf16)
    scopy.wait_recv()
    member = own_half.astype(f32) + half_recv[...].astype(f32)
    ret_send[...] = member[: n * base].reshape(n, base, halfw).astype(bf16)
    for k in range(extra):
        first = n * (base + k)
        for c in range(chunks):
            ext_wide[0, :, k * chunks + c, :] = member[first : first + n, c * 128 : (c + 1) * 128]
    rex_send[...] = ext_wide[0].astype(bf16)
    mcopies, xcopies = [], []
    for d in range(1, n):
        mcopies.append(
            remote(ret_send.at[d], ret_recv.at[d - 1], m_send.at[d], m_recv.at[d], ring(-d), tp)
        )
        xcopies.append(
            remote(
                rex_send.at[d], rex_recv.at[d - 1], m_send.at[n + d], m_recv.at[n + d], ring(-d), tp
            )
        )

    remote(dd_ref, weights.at[2, 1 - x], w_send.at[2], w_recv.at[2], pair, tp, go=False).wait_recv()
    for d in range(1, nz):
        hcopies[d - 1].wait_recv()
    owner = lax.div(z, pos_count)
    place = lax.rem(z, pos_count)
    hid_in = hid_all[...].reshape(nz * toks, hidden)
    for i in range(2):
        part = jnp.dot(hid_in, weights[2, i], preferred_element_type=f32).astype(bf16)
        down_send[:, :, i * fh : (i + 1) * fh] = part.reshape(nz, toks, fh)
    for d in range(1, nz):
        remote(
            down_send.at[d],
            down_recv.at[place, tp],
            d_send.at[d],
            d_recv.at[place, tp],
            line(-d),
            owner,
        )

    def sibling_copy():
        return remote(
            down_send.at[0],
            down_recv.at[place, tp],
            d_send.at[0],
            d_recv.at[place, tp],
            ep,
            sib,
            go=False,
        )

    @pl.when(owner != tp)
    def _():
        sibling_copy().start()

    @pl.when(owner == tp)
    def _():
        down_recv[place, tp] = down_send[0]

    total = ret_send[0].astype(f32)
    ext_total = rex_send[0].astype(f32)
    for d in range(1, n):
        mcopies[d - 1].wait_recv()
        xcopies[d - 1].wait_recv()
        total = total + ret_recv[d - 1].astype(f32)
        ext_total = ext_total + rex_recv[d - 1].astype(f32)
    if spad > base:
        row_id = lax.broadcasted_iota(jnp.int32, (spad - base, halfw), 0)
        tail = jnp.zeros((spad - base, halfw), f32)
        for k in range(extra):
            row = jnp.concatenate(
                [ext_total[k * chunks + c : k * chunks + c + 1, :] for c in range(chunks)], 1
            )
            tail = jnp.where(row_id == k, row, tail)
        total = jnp.concatenate([total, tail], 0)
    spread = jnp.where(match, table[8:9, :], 0.0)[:, :spad]
    combined = jnp.dot(
        spread, total, preferred_element_type=f32, precision=lax.Precision.HIGHEST
    )
    for p in range(pos_count):
        for t in range(2):

            @pl.when(jnp.logical_or(tp * pos_count + p != z, tp != t))
            def _():
                wait_on(d_send.at[0], d_recv.at[p, t], down_recv.at[p, t])

        cols = slice(p * feat, (p + 1) * feat)
        dense = down_recv[p, 0].astype(f32) + down_recv[p, 1].astype(f32)
        scale = 1.0 / (1.0 + jnp.exp(-bg_ref[:, cols]))
        out_ref[:, cols] = (combined[:, cols] + scale * dense).astype(bf16)

    for copy in sends:
        copy.wait_send()

    @pl.when(owner != tp)
    def _():
        sibling_copy().wait_send()


def fused_local(n, *args):
    tokens, chosen, dense_gate, branch_gate = args[0], args[1], args[6], args[9]
    toks, width = tokens.shape
    nz = n // 2
    feat = width // nz
    slots = chosen.shape[2]
    base = slots // 8 * 8
    lines = (slots - base) * (width // 256)
    every = -(-n * slots // 16) * 16
    hid = dense_gate.shape[1]
    units = args[3].shape[1]
    bf16 = jnp.bfloat16
    vmem = pl.BlockSpec(memory_space=pltpu.VMEM)
    hbm = pl.BlockSpec(memory_space=pl.ANY)
    dma = pltpu.SemaphoreType.DMA
    scratch = [
        pltpu.VMEM((width, units), bf16),
        pltpu.VMEM((width, units), bf16),
        pltpu.VMEM((units, width), bf16),
        pltpu.VMEM((3, 2) + dense_gate.shape, bf16),
        pltpu.VMEM((nz, toks, feat), bf16),
        pltpu.VMEM((16, 128), jnp.float32),
        pltpu.VMEM((2, n, base, width // 2), bf16),
        pltpu.VMEM((2, n, lines, 128), bf16),
        pltpu.VMEM((2, n, lines, 128), jnp.float32),
        pltpu.VMEM((nz - 1, 2, toks, hid), bf16),
        pltpu.VMEM((nz - 1, 2, toks, hid), bf16),
        pltpu.VMEM((nz, toks, hid), bf16),
        pltpu.VMEM((nz, toks, feat), bf16),
        pltpu.VMEM((nz // 2, 2, toks, feat), bf16),
        pltpu.VMEM((every, width // 2), bf16),
        pltpu.VMEM((every, width // 2), bf16),
        pltpu.VMEM((n, base, width // 2), bf16),
        pltpu.VMEM((n - 1, base, width // 2), bf16),
        pltpu.VMEM((n, lines, 128), bf16),
        pltpu.VMEM((n - 1, lines, 128), bf16),
        dma((3,)),
        dma((3,)),
        dma((3,)),
        dma((nz,)),
        dma((nz,)),
        dma((nz,)),
        dma((nz,)),
        dma((2 * n,)),
        dma((2 * n,)),
        dma((2 * n,)),
        dma((2 * n,)),
        dma((nz,)),
        dma((nz,)),
        dma((nz,)),
        dma((nz,)),
        dma((nz,)),
        dma((nz // 2, 2)),
        dma,
        dma,
        dma((2 * n,)),
        dma((2 * n,)),
    ]
    return pl.pallas_call(
        functools.partial(fused_kernel, n),
        out_shape=jax.ShapeDtypeStruct((toks, width // 2), bf16),
        in_specs=[vmem] * 3 + [hbm] * 3 + [vmem] * 4,
        out_specs=vmem,
        scratch_shapes=scratch,
        compiler_params=pltpu.CompilerParams(collective_id=0, has_side_effects=True),
    )(*args[:9], branch_gate.reshape(1, -1))


def local(*args):
    n = lax.axis_size("ep")
    tokens, chosen, dense_gate = args[0], args[1], args[6]
    width = tokens.shape[1]
    square = dense_gate.shape[0] == dense_gate.shape[1] == args[8].shape[1]
    fits = chosen.shape[0] == 1 and n % 4 == 0 and square
    fits = fits and (width // n) % 128 == 0 and tokens.shape[0] % 32 == 0
    fits = fits and chosen.shape[2] > 8 and chosen.shape[2] % 8 != 0 and width % 2048 == 0
    fits = fits and chosen.shape[2] <= 128 and lax.axis_size("tp") == 2
    return fused_local(n, *args) if fits else plain_local(*args)


def plain_local(
    tokens,
    chosen,
    route_weight,
    expert_gate,
    expert_up,
    expert_down,
    dense_gate,
    dense_up,
    dense_down,
    branch_gate,
):
    ep_count = lax.axis_size("ep")
    experts = chosen.shape[0]
    slots = chosen.shape[2]
    tok_local = tokens.shape[0]
    width = tokens.shape[1]
    picked = chosen[:, 0, :]
    filled = picked >= 0
    token_rows = jnp.take(tokens, jnp.maximum(picked, 0).reshape(-1), axis=0).reshape(
        experts, slots, width
    )
    token_rows = jnp.where(filled[:, :, None], token_rows, jnp.zeros((), jnp.bfloat16))
    send_width = token_rows.shape[2]
    piece = send_width // 8
    split_rows = jnp.transpose(token_rows.reshape(experts, slots, 8, piece), (0, 2, 1, 3)).reshape(
        ep_count, slots, piece
    )
    own_piece = lax.all_to_all(split_rows, "ep", split_axis=0, concat_axis=0, tiled=True)
    member = lax.axis_index("ep") % 8
    current = own_piece[:, :, None, :]
    partner = swapped(current, "ep", 0)
    current = join_pieces(current, partner, member % 2 == 1)
    partner = swapped(current, "ep", 1)
    current = join_pieces(current, partner, member // 2 % 2 == 1)
    partner = swapped(current, "ep", 2)
    current = join_pieces(current, partner, member // 4 == 1)
    received = current.reshape(ep_count, slots, send_width)
    hidden = expert_hidden(received, gate_cols=expert_gate, up_cols=expert_up)
    flat_hidden = hidden.reshape(ep_count * slots, -1)
    shard_rows = expert_down
    member_sums = lax.psum_scatter(
        lax.dot_general(
            shard_rows, flat_hidden, (((0,), (1,)), ((), ())), preferred_element_type=jnp.float32
        ).astype(jnp.bfloat16),
        "tp",
        scatter_dimension=0,
        tiled=True,
    )
    returned = lax.all_to_all(member_sums, "ep", split_axis=1, concat_axis=1, tiled=True)
    summed = returned.astype(jnp.float32).reshape(width // 2, experts, 8, slots).sum(axis=2)
    positions = lax.broadcasted_iota(jnp.int32, (experts, slots, tok_local), 2)
    weights_table = jnp.where(picked[:, :, None] == positions, route_weight[:, 0, :, None], 0.0)
    combined = jnp.einsum("fek,ekt->tf", summed, weights_table, precision=lax.Precision.HIGHEST)
    shard_rows = (
        lax.all_gather(dense_gate, "ep", axis=0, tiled=True),
        lax.all_gather(dense_up, "ep", axis=0, tiled=True),
    )
    gate_dense = jnp.dot(tokens, shard_rows[0], preferred_element_type=jnp.float32)
    up_dense = jnp.dot(tokens, shard_rows[1], preferred_element_type=jnp.float32)
    dense_hidden = (jax.nn.silu(gate_dense) * up_dense).astype(jnp.bfloat16)
    dense_terms = jnp.dot(
        dense_hidden,
        lax.all_gather(dense_down, "ep", axis=1, tiled=True),
        preferred_element_type=jnp.float32,
    )
    dense_sum = lax.psum_scatter(
        dense_terms.astype(jnp.bfloat16), "tp", scatter_dimension=1, tiled=True
    ).astype(jnp.float32)
    return (combined + jax.nn.sigmoid(branch_gate)[None, :] * dense_sum).astype(jnp.bfloat16)


def solution(mesh):
    return jax.shard_map(
        local,
        mesh=mesh,
        in_specs=(
            P(("grp", "ep"), None),
            P(None, ("grp", "ep"), None),
            P(None, ("grp", "ep"), None),
            P(None, ("ep", "tp")),
            P(None, ("ep", "tp")),
            P(("ep", "tp"), None),
            P("ep", "tp"),
            P("ep", "tp"),
            P("tp", "ep"),
            P("tp"),
        ),
        out_specs=P(("grp", "ep"), "tp"),
        check_vma=False,
    )
```

```python
import functools

import jax
import jax.numpy as jnp
from jax import lax
from jax.experimental import pallas as pl
from jax.experimental.pallas import tpu as pltpu
from jax.sharding import PartitionSpec as P

MESH = pl.DeviceIdType.MESH


def swapped(block, axis, apart):
    count = lax.axis_size(axis)
    route = []
    for low in range(count):
        high = low | 1 << apart
        if high != low and high < count:
            route += [(low, high), (high, low)]
    return lax.ppermute(block, axis, route)


def expert_hidden(received, gate_cols, up_cols):
    flat_rows = received.reshape(-1, received.shape[-1])
    gate_act = jnp.dot(flat_rows, gate_cols, preferred_element_type=jnp.float32)
    up_act = jnp.dot(flat_rows, up_cols, preferred_element_type=jnp.float32)
    hidden = (jax.nn.silu(gate_act) * up_act).astype(jnp.bfloat16)
    return hidden.reshape(received.shape[0], received.shape[1], gate_cols.shape[1])


def join_pieces(mine, theirs, upper):
    return jnp.where(upper, jnp.concatenate([theirs, mine], 2), jnp.concatenate([mine, theirs], 2))


def fused_kernel(
    n,
    tok_hbm,
    chosen_ref,
    route_ref,
    eg_hbm,
    eu_hbm,
    ed_hbm,
    dg_hbm,
    du_hbm,
    dd_hbm,
    bg_ref,
    out_ref,
    tok_ref,
    eg,
    eu,
    ed,
    weights,
    tok_all,
    table,
    rows_all,
    ext_all,
    ext_wide,
    part_send,
    part_recv,
    hid_all,
    down_send,
    down_recv,
    pre_send,
    pre_recv,
    half_send,
    half_recv,
    ret_send,
    ret_recv,
    rex_send,
    rex_recv,
    local_sem,
    w_send,
    w_recv,
    t_send,
    t_recv,
    tf_send,
    tf_recv,
    r_send,
    r_recv,
    rf_send,
    rf_recv,
    p_send,
    p_recv,
    h_send,
    h_recv,
    d_send,
    d_recv,
    s_send,
    s_recv,
    q_send,
    q_recv,
    m_send,
    m_recv,
):
    f32, bf16 = jnp.float32, jnp.bfloat16
    ep, tp = lax.axis_index("ep"), lax.axis_index("tp")
    sib = 1 - tp
    nz = n // 2
    x, z = lax.rem(ep, 2), lax.div(ep, 2)
    toks, width = tok_ref.shape
    feat = width // nz
    halfw = width // 2
    base = rows_all.shape[2]
    chunks = halfw // 128
    hidden = weights.shape[3]
    pos_count = nz // 2

    def line(d):
        return lax.rem(z + d + nz, nz) * 2 + x

    def ring(d):
        return lax.rem(ep + d + n, n)

    sends = []

    def remote(src, dst, ssem, rsem, to_ep, to_tp, go=True):
        copy = pltpu.make_async_remote_copy(
            src_ref=src,
            dst_ref=dst,
            send_sem=ssem,
            recv_sem=rsem,
            device_id={"ep": to_ep, "tp": to_tp},
            device_id_type=MESH,
        )
        if go:
            copy.start()
            sends.append(copy)
        return copy

    loads = []
    plan = ((eg_hbm, eg), (eu_hbm, eu), (ed_hbm, ed), (tok_hbm, tok_ref))
    plan += tuple((w, weights.at[i, x]) for i, w in enumerate((dg_hbm, du_hbm, dd_hbm)))
    for i, (src, dst) in enumerate(plan[3:] + plan[:3]):
        load = pltpu.make_async_copy(src, dst, local_sem.at[i])
        load.start()
        loads.append(load)
    early, loads = loads[:4], loads[4:]

    barrier = pltpu.get_barrier_semaphore()
    for d in range(1, n):
        pl.semaphore_signal(
            barrier, inc=1, device_id={"ep": ring(d), "tp": tp}, device_id_type=MESH
        )
    for d in range(nz):
        pl.semaphore_signal(
            barrier, inc=1, device_id={"ep": line(d), "tp": sib}, device_id_type=MESH
        )

    table[...] = jnp.full(table.shape, -1.0, f32)
    slots = chosen_ref.shape[2]
    extra = slots - base
    spad = -(-slots // 16) * 16
    table[0:1, 0:slots] = chosen_ref[0].astype(f32)
    table[8:9, 0:slots] = route_ref[0]
    token_id = lax.broadcasted_iota(jnp.int32, (toks, table.shape[1]), 0).astype(f32)
    match = token_id == table[0:1, :]
    onehot = jnp.where(match, 1.0, 0.0).astype(f32)
    early[0].wait()
    pick = onehot.T[:spad].astype(bf16)
    picked = jnp.dot(pick, tok_ref[...], preferred_element_type=f32)
    for h in range(2):
        rows_all[h, 0] = picked[:base, h * halfw : (h + 1) * halfw].astype(bf16)
        pieces = [
            picked[base + k : base + k + 1, h * halfw + c * 128 : h * halfw + (c + 1) * 128]
            for k in range(extra)
            for c in range(chunks)
        ]
        ext_all[h, 0] = jnp.concatenate(pieces, 0).astype(bf16)

    pl.semaphore_wait(barrier, n - 1 + nz)

    th = toks // 2
    mine = pl.ds(pl.multiple_of(tp * th, th), th)
    theirs = pl.ds(pl.multiple_of(sib * th, th), th)
    tcopies = []
    for d in range(1, nz):
        cols = pl.ds(pl.multiple_of(lax.rem(z + d, nz) * feat, feat), feat)
        tcopies.append(
            remote(
                tok_ref.at[mine, cols],
                tok_all.at[d, mine],
                t_send.at[d],
                t_recv.at[d],
                line(d),
                tp,
            )
        )
    pair = ep + 1 - 2 * x
    for i in range(3):
        early[1 + i].wait()
        own = weights.at[i, x]
        remote(own, own, w_send.at[i], w_recv.at[i], pair, tp)
    rcopies, ecopies = [], []
    for d in range(1, n):
        rcopies.append(
            remote(
                rows_all.at[tp, 0], rows_all.at[tp, d], r_send.at[d], r_recv.at[d], ring(d), tp
            )
        )
        ecopies.append(
            remote(
                ext_all.at[tp, 0],
                ext_all.at[tp, d],
                r_send.at[n + d],
                r_recv.at[n + d],
                ring(d),
                tp,
            )
        )

    own_cols = pl.ds(pl.multiple_of(z * feat, feat), feat)
    tok_all[0] = tok_ref[:, own_cols]

    for d in range(1, nz):
        tcopies[d - 1].wait_recv()
        remote(
            tok_all.at[d, mine], tok_all.at[d, mine], tf_send.at[d], tf_recv.at[d], ep, sib
        )
    wait_at = lambda dst, ssem, rsem: remote(dst, dst, ssem, rsem, ep, sib, go=False).wait_recv()

    def wait_on(ssem, rsem, dst):
        wait_at(dst, ssem, rsem)

    for i in range(2):
        remote(weights.at[i, x], weights.at[i, 1 - x], w_send.at[i], w_recv.at[i], pair, tp, go=False).wait_recv()
    for d in range(1, nz):
        wait_on(tf_send.at[d], tf_recv.at[d], tok_all.at[d, theirs])
    toks_in = tok_all[...].reshape(nz * toks, feat)
    fh = feat // 2
    sums = []
    for i in range(2):
        total = jnp.dot(toks_in[:, :fh], weights[i, 0], preferred_element_type=f32) + jnp.dot(
            toks_in[:, fh:], weights[i, 1], preferred_element_type=f32
        )
        sums.append(total[:toks])
        for d in range(1, nz):
            part_send[d - 1, i] = total[d * toks : (d + 1) * toks].astype(bf16)
    pcopies = []
    for d in range(1, nz):
        pcopies.append(
            remote(
                part_send.at[d - 1], part_recv.at[d - 1], p_send.at[d], p_recv.at[d], line(-d), tp
            )
        )

    for d in range(1, n):
        rcopies[d - 1].wait_recv()
        remote(
            rows_all.at[tp, d], rows_all.at[tp, d], rf_send.at[d], rf_recv.at[d], ep, sib
        )
        ecopies[d - 1].wait_recv()
        remote(
            ext_all.at[tp, d], ext_all.at[tp, d], rf_send.at[n + d], rf_recv.at[n + d], ep, sib
        )
    for load in loads[:2]:
        load.wait()
    for d in range(1, n):
        wait_on(rf_send.at[d], rf_recv.at[d], rows_all.at[sib, d])
        wait_on(rf_send.at[n + d], rf_recv.at[n + d], ext_all.at[sib, d])
    ext_wide[...] = ext_all[...].astype(f32)
    every = half_send.shape[0]

    def stacked(h):
        parts = [rows_all[h].astype(f32).reshape(n * base, halfw)]
        for k in range(extra):
            parts.append(
                jnp.concatenate([ext_wide[h, :, k * chunks + c, :] for c in range(chunks)], 1)
            )
        if every > n * slots:
            parts.append(jnp.zeros((every - n * slots, halfw), f32))
        return jnp.concatenate(parts, 0).astype(bf16)

    low, high = stacked(0), stacked(1)

    def project(w):
        return jnp.dot(low, w[:halfw], preferred_element_type=f32) + jnp.dot(
            high, w[halfw:], preferred_element_type=f32
        )

    gate = project(eg)
    up = project(eu)
    act = (gate / (1.0 + jnp.exp(-gate)) * up).astype(bf16)
    loads[2].wait()
    off = pl.ds(pl.multiple_of(sib * halfw, halfw), halfw)
    keep = pl.ds(pl.multiple_of(tp * halfw, halfw), halfw)
    half_send[...] = jnp.dot(act, ed[:, off], preferred_element_type=f32).astype(bf16)
    scopy = remote(half_send, half_recv, s_send, s_recv, ep, sib)

    for d in range(1, nz):
        pcopies[d - 1].wait_recv()
        sums = [sums[i] + part_recv[d - 1, i].astype(f32) for i in range(2)]
    dense_hidden = (sums[0] / (1.0 + jnp.exp(-sums[0])) * sums[1]).astype(bf16)
    hid_all[0] = dense_hidden
    hcopies = []
    for d in range(1, nz):
        hcopies.append(
            remote(hid_all.at[0], hid_all.at[d], h_send.at[d], h_recv.at[d], line(d), tp)
        )

    own_half = jnp.dot(act, ed[:, keep], preferred_element_type=f32).astype(bf16)
    scopy.wait_recv()
    member = own_half.astype(f32) + half_recv[...].astype(f32)
    ret_send[...] = member[: n * base].reshape(n, base, halfw).astype(bf16)
    for k in range(extra):
        first = n * (base + k)
        for c in range(chunks):
            ext_wide[0, :, k * chunks + c, :] = member[first : first + n, c * 128 : (c + 1) * 128]
    rex_send[...] = ext_wide[0].astype(bf16)
    mcopies, xcopies = [], []
    for d in range(1, n):
        mcopies.append(
            remote(ret_send.at[d], ret_recv.at[d - 1], m_send.at[d], m_recv.at[d], ring(-d), tp)
        )
        xcopies.append(
            remote(
                rex_send.at[d], rex_recv.at[d - 1], m_send.at[n + d], m_recv.at[n + d], ring(-d), tp
            )
        )

    remote(weights.at[2, x], weights.at[2, 1 - x], w_send.at[2], w_recv.at[2], pair, tp, go=False).wait_recv()
    for d in range(1, nz):
        hcopies[d - 1].wait_recv()
    owner = lax.div(z, pos_count)
    place = lax.rem(z, pos_count)
    hid_in = hid_all[...].reshape(nz * toks, hidden)
    away = jnp.dot(hid_in, weights[2, sib], preferred_element_type=f32)
    pre_send[...] = away.astype(bf16)
    qcopy = remote(pre_send, pre_recv, q_send, q_recv, ep, sib)
    part = jnp.dot(hid_in, weights[2, tp], preferred_element_type=f32)
    qcopy.wait_recv()
    part = part + pre_recv[...].astype(f32)
    down_send[...] = part.astype(bf16).reshape(nz, toks, fh)
    for d in range(1, nz):
        remote(
            down_send.at[d],
            down_recv.at[place, tp],
            d_send.at[d],
            d_recv.at[place, tp],
            line(-d),
            owner,
        )

    def sibling_copy():
        return remote(
            down_send.at[0],
            down_recv.at[place, tp],
            d_send.at[0],
            d_recv.at[place, tp],
            ep,
            sib,
            go=False,
        )

    @pl.when(owner != tp)
    def _():
        sibling_copy().start()

    @pl.when(owner == tp)
    def _():
        down_recv[place, tp] = down_send[0]

    total = ret_send[0].astype(f32)
    ext_total = rex_send[0].astype(f32)
    for d in range(1, n):
        mcopies[d - 1].wait_recv()
        xcopies[d - 1].wait_recv()
        total = total + ret_recv[d - 1].astype(f32)
        ext_total = ext_total + rex_recv[d - 1].astype(f32)
    if spad > base:
        row_id = lax.broadcasted_iota(jnp.int32, (spad - base, halfw), 0)
        tail = jnp.zeros((spad - base, halfw), f32)
        for k in range(extra):
            row = jnp.concatenate(
                [ext_total[k * chunks + c : k * chunks + c + 1, :] for c in range(chunks)], 1
            )
            tail = jnp.where(row_id == k, row, tail)
        total = jnp.concatenate([total, tail], 0)
    spread = jnp.where(match, table[8:9, :], 0.0)[:, :spad]
    combined = jnp.dot(
        spread, total, preferred_element_type=f32, precision=lax.Precision.HIGHEST
    )
    for p in range(pos_count):
        for t in range(2):

            @pl.when(jnp.logical_or(tp * pos_count + p != z, tp != t))
            def _():
                wait_on(d_send.at[0], d_recv.at[p, t], down_recv.at[p, t])

        for t in range(2):
            cols = slice(p * feat + t * fh, p * feat + (t + 1) * fh)
            dense = down_recv[p, t].astype(f32)
            scale = 1.0 / (1.0 + jnp.exp(-bg_ref[:, cols]))
            out_ref[:, cols] = (combined[:, cols] + scale * dense).astype(bf16)

    for copy in sends:
        copy.wait_send()

    @pl.when(owner != tp)
    def _():
        sibling_copy().wait_send()


def fused_local(n, *args):
    tokens, chosen, dense_gate, branch_gate = args[0], args[1], args[6], args[9]
    toks, width = tokens.shape
    nz = n // 2
    feat = width // nz
    slots = chosen.shape[2]
    base = slots // 8 * 8
    lines = (slots - base) * (width // 256)
    every = -(-n * slots // 16) * 16
    hid = dense_gate.shape[1]
    units = args[3].shape[1]
    bf16 = jnp.bfloat16
    vmem = pl.BlockSpec(memory_space=pltpu.VMEM)
    hbm = pl.BlockSpec(memory_space=pl.ANY)
    dma = pltpu.SemaphoreType.DMA
    scratch = [
        pltpu.VMEM((toks, width), bf16),
        pltpu.VMEM((width, units), bf16),
        pltpu.VMEM((width, units), bf16),
        pltpu.VMEM((units, width), bf16),
        pltpu.VMEM((3, 2) + dense_gate.shape, bf16),
        pltpu.VMEM((nz, toks, feat), bf16),
        pltpu.VMEM((16, 128), jnp.float32),
        pltpu.VMEM((2, n, base, width // 2), bf16),
        pltpu.VMEM((2, n, lines, 128), bf16),
        pltpu.VMEM((2, n, lines, 128), jnp.float32),
        pltpu.VMEM((nz - 1, 2, toks, hid), bf16),
        pltpu.VMEM((nz - 1, 2, toks, hid), bf16),
        pltpu.VMEM((nz, toks, hid), bf16),
        pltpu.VMEM((nz, toks, feat // 2), bf16),
        pltpu.VMEM((nz // 2, 2, toks, feat // 2), bf16),
        pltpu.VMEM((nz * toks, feat // 2), bf16),
        pltpu.VMEM((nz * toks, feat // 2), bf16),
        pltpu.VMEM((every, width // 2), bf16),
        pltpu.VMEM((every, width // 2), bf16),
        pltpu.VMEM((n, base, width // 2), bf16),
        pltpu.VMEM((n - 1, base, width // 2), bf16),
        pltpu.VMEM((n, lines, 128), bf16),
        pltpu.VMEM((n - 1, lines, 128), bf16),
        dma((7,)),
        dma((3,)),
        dma((3,)),
        dma((nz,)),
        dma((nz,)),
        dma((nz,)),
        dma((nz,)),
        dma((2 * n,)),
        dma((2 * n,)),
        dma((2 * n,)),
        dma((2 * n,)),
        dma((nz,)),
        dma((nz,)),
        dma((nz,)),
        dma((nz,)),
        dma((nz,)),
        dma((nz // 2, 2)),
        dma,
        dma,
        dma,
        dma,
        dma((2 * n,)),
        dma((2 * n,)),
    ]
    return pl.pallas_call(
        functools.partial(fused_kernel, n),
        out_shape=jax.ShapeDtypeStruct((toks, width // 2), bf16),
        in_specs=[hbm] + [vmem] * 2 + [hbm] * 6 + [vmem],
        out_specs=vmem,
        scratch_shapes=scratch,
        compiler_params=pltpu.CompilerParams(collective_id=0, has_side_effects=True),
    )(*args[:9], branch_gate.reshape(1, -1))


def local(*args):
    n = lax.axis_size("ep")
    tokens, chosen, dense_gate = args[0], args[1], args[6]
    width = tokens.shape[1]
    square = dense_gate.shape[0] == dense_gate.shape[1] == args[8].shape[1]
    fits = chosen.shape[0] == 1 and n % 4 == 0 and square
    fits = fits and (width // n) % 128 == 0 and tokens.shape[0] % 32 == 0
    fits = fits and chosen.shape[2] > 8 and chosen.shape[2] % 8 != 0 and width % 2048 == 0
    fits = fits and chosen.shape[2] <= 128 and lax.axis_size("tp") == 2
    return fused_local(n, *args) if fits else plain_local(*args)


def plain_local(
    tokens,
    chosen,
    route_weight,
    expert_gate,
    expert_up,
    expert_down,
    dense_gate,
    dense_up,
    dense_down,
    branch_gate,
):
    ep_count = lax.axis_size("ep")
    experts = chosen.shape[0]
    slots = chosen.shape[2]
    tok_local = tokens.shape[0]
    width = tokens.shape[1]
    picked = chosen[:, 0, :]
    filled = picked >= 0
    token_rows = jnp.take(tokens, jnp.maximum(picked, 0).reshape(-1), axis=0).reshape(
        experts, slots, width
    )
    token_rows = jnp.where(filled[:, :, None], token_rows, jnp.zeros((), jnp.bfloat16))
    send_width = token_rows.shape[2]
    piece = send_width // 8
    split_rows = jnp.transpose(token_rows.reshape(experts, slots, 8, piece), (0, 2, 1, 3)).reshape(
        ep_count, slots, piece
    )
    own_piece = lax.all_to_all(split_rows, "ep", split_axis=0, concat_axis=0, tiled=True)
    member = lax.axis_index("ep") % 8
    current = own_piece[:, :, None, :]
    partner = swapped(current, "ep", 0)
    current = join_pieces(current, partner, member % 2 == 1)
    partner = swapped(current, "ep", 1)
    current = join_pieces(current, partner, member // 2 % 2 == 1)
    partner = swapped(current, "ep", 2)
    current = join_pieces(current, partner, member // 4 == 1)
    received = current.reshape(ep_count, slots, send_width)
    hidden = expert_hidden(received, gate_cols=expert_gate, up_cols=expert_up)
    flat_hidden = hidden.reshape(ep_count * slots, -1)
    shard_rows = expert_down
    member_sums = lax.psum_scatter(
        lax.dot_general(
            shard_rows, flat_hidden, (((0,), (1,)), ((), ())), preferred_element_type=jnp.float32
        ).astype(jnp.bfloat16),
        "tp",
        scatter_dimension=0,
        tiled=True,
    )
    returned = lax.all_to_all(member_sums, "ep", split_axis=1, concat_axis=1, tiled=True)
    summed = returned.astype(jnp.float32).reshape(width // 2, experts, 8, slots).sum(axis=2)
    positions = lax.broadcasted_iota(jnp.int32, (experts, slots, tok_local), 2)
    weights_table = jnp.where(picked[:, :, None] == positions, route_weight[:, 0, :, None], 0.0)
    combined = jnp.einsum("fek,ekt->tf", summed, weights_table, precision=lax.Precision.HIGHEST)
    shard_rows = (
        lax.all_gather(dense_gate, "ep", axis=0, tiled=True),
        lax.all_gather(dense_up, "ep", axis=0, tiled=True),
    )
    gate_dense = jnp.dot(tokens, shard_rows[0], preferred_element_type=jnp.float32)
    up_dense = jnp.dot(tokens, shard_rows[1], preferred_element_type=jnp.float32)
    dense_hidden = (jax.nn.silu(gate_dense) * up_dense).astype(jnp.bfloat16)
    dense_terms = jnp.dot(
        dense_hidden,
        lax.all_gather(dense_down, "ep", axis=1, tiled=True),
        preferred_element_type=jnp.float32,
    )
    dense_sum = lax.psum_scatter(
        dense_terms.astype(jnp.bfloat16), "tp", scatter_dimension=1, tiled=True
    ).astype(jnp.float32)
    return (combined + jax.nn.sigmoid(branch_gate)[None, :] * dense_sum).astype(jnp.bfloat16)


def solution(mesh):
    return jax.shard_map(
        local,
        mesh=mesh,
        in_specs=(
            P(("grp", "ep"), None),
            P(None, ("grp", "ep"), None),
            P(None, ("grp", "ep"), None),
            P(None, ("ep", "tp")),
            P(None, ("ep", "tp")),
            P(("ep", "tp"), None),
            P("ep", "tp"),
            P("ep", "tp"),
            P("tp", "ep"),
            P("tp"),
        ),
        out_specs=P(("grp", "ep"), "tp"),
        check_vma=False,
    )
```

```python
import functools

import jax
import jax.numpy as jnp
from jax import lax
from jax.experimental import pallas as pl
from jax.experimental.pallas import tpu as pltpu
from jax.sharding import PartitionSpec as P

MESH = pl.DeviceIdType.MESH


def swapped(block, axis, apart):
    count = lax.axis_size(axis)
    route = []
    for low in range(count):
        high = low | 1 << apart
        if high != low and high < count:
            route += [(low, high), (high, low)]
    return lax.ppermute(block, axis, route)


def expert_hidden(received, gate_cols, up_cols):
    flat_rows = received.reshape(-1, received.shape[-1])
    gate_act = jnp.dot(flat_rows, gate_cols, preferred_element_type=jnp.float32)
    up_act = jnp.dot(flat_rows, up_cols, preferred_element_type=jnp.float32)
    hidden = (jax.nn.silu(gate_act) * up_act).astype(jnp.bfloat16)
    return hidden.reshape(received.shape[0], received.shape[1], gate_cols.shape[1])


def join_pieces(mine, theirs, upper):
    return jnp.where(upper, jnp.concatenate([theirs, mine], 2), jnp.concatenate([mine, theirs], 2))


def fused_kernel(
    n,
    tok_hbm,
    chosen_ref,
    route_ref,
    eg_hbm,
    eu_hbm,
    ed_hbm,
    dg_hbm,
    du_hbm,
    dd_hbm,
    bg_ref,
    out_ref,
    tok_ref,
    eg,
    eu,
    ed,
    weights,
    tok_all,
    table,
    rows_all,
    ext_all,
    ext_wide,
    part_send,
    part_recv,
    hid_all,
    down_send,
    down_recv,
    pre_send,
    pre_recv,
    half_send,
    half_recv,
    ret_send,
    ret_recv,
    rex_send,
    rex_recv,
    local_sem,
    w_send,
    w_recv,
    t_send,
    t_recv,
    tf_send,
    tf_recv,
    r_send,
    r_recv,
    rf_send,
    rf_recv,
    p_send,
    p_recv,
    h_send,
    h_recv,
    d_send,
    d_recv,
    s_send,
    s_recv,
    q_send,
    q_recv,
    m_send,
    m_recv,
):
    f32, bf16 = jnp.float32, jnp.bfloat16
    ep, tp = lax.axis_index("ep"), lax.axis_index("tp")
    sib = 1 - tp
    nz = n // 2
    x, z = lax.rem(ep, 2), lax.div(ep, 2)
    toks, width = tok_ref.shape
    feat = width // nz
    halfw = width // 2
    base = rows_all.shape[2]
    chunks = halfw // 128
    hidden = weights.shape[3]
    pos_count = nz // 2

    def line(d):
        return lax.rem(z + d + nz, nz) * 2 + x

    def ring(d):
        return lax.rem(ep + d + n, n)

    sends = []

    def remote(src, dst, ssem, rsem, to_ep, to_tp, go=True):
        copy = pltpu.make_async_remote_copy(
            src_ref=src,
            dst_ref=dst,
            send_sem=ssem,
            recv_sem=rsem,
            device_id={"ep": to_ep, "tp": to_tp},
            device_id_type=MESH,
        )
        if go:
            copy.start()
            sends.append(copy)
        return copy

    loads = []
    plan = ((eg_hbm, eg), (eu_hbm, eu), (ed_hbm, ed), (tok_hbm, tok_ref))
    plan += tuple((w, weights.at[i, x]) for i, w in enumerate((dg_hbm, du_hbm, dd_hbm)))
    for i, (src, dst) in enumerate(plan[3:] + plan[:3]):
        load = pltpu.make_async_copy(src, dst, local_sem.at[i])
        load.start()
        loads.append(load)
    early, loads = loads[:4], loads[4:]

    barrier = pltpu.get_barrier_semaphore()
    for d in range(1, n):
        pl.semaphore_signal(
            barrier, inc=1, device_id={"ep": ring(d), "tp": tp}, device_id_type=MESH
        )
    for d in range(nz):
        pl.semaphore_signal(
            barrier, inc=1, device_id={"ep": line(d), "tp": sib}, device_id_type=MESH
        )

    table[...] = jnp.full(table.shape, -1.0, f32)
    slots = chosen_ref.shape[2]
    extra = slots - base
    spad = -(-slots // 16) * 16
    table[0:1, 0:slots] = chosen_ref[0].astype(f32)
    table[8:9, 0:slots] = route_ref[0]
    token_id = lax.broadcasted_iota(jnp.int32, (toks, table.shape[1]), 0).astype(f32)
    match = token_id == table[0:1, :]
    onehot = jnp.where(match, 1.0, 0.0).astype(f32)
    early[0].wait()
    pick = onehot.T[:spad].astype(bf16)
    picked = jnp.dot(pick, tok_ref[...], preferred_element_type=f32)
    for h in range(2):
        rows_all[h, 0] = picked[:base, h * halfw : (h + 1) * halfw].astype(bf16)
        pieces = [
            picked[base + k : base + k + 1, h * halfw + c * 128 : h * halfw + (c + 1) * 128]
            for k in range(extra)
            for c in range(chunks)
        ]
        ext_all[h, 0] = jnp.concatenate(pieces, 0).astype(bf16)

    pl.semaphore_wait(barrier, n - 1 + nz)

    th = toks // 2
    mine = pl.ds(pl.multiple_of(tp * th, th), th)
    theirs = pl.ds(pl.multiple_of(sib * th, th), th)
    tcopies = []
    for d in range(1, nz):
        cols = pl.ds(pl.multiple_of(lax.rem(z + d, nz) * feat, feat), feat)
        tcopies.append(
            remote(
                tok_ref.at[mine, cols],
                tok_all.at[d, mine],
                t_send.at[d],
                t_recv.at[d],
                line(d),
                tp,
            )
        )
    pair = ep + 1 - 2 * x
    for i in range(3):
        early[1 + i].wait()
        own = weights.at[i, x]
        remote(own, own, w_send.at[i], w_recv.at[i], pair, tp)
    rcopies, ecopies = [], []
    for d in range(1, n):
        rcopies.append(
            remote(
                rows_all.at[tp, 0], rows_all.at[tp, d], r_send.at[d], r_recv.at[d], ring(d), tp
            )
        )
        ecopies.append(
            remote(
                ext_all.at[tp, 0],
                ext_all.at[tp, d],
                r_send.at[n + d],
                r_recv.at[n + d],
                ring(d),
                tp,
            )
        )

    own_cols = pl.ds(pl.multiple_of(z * feat, feat), feat)
    tok_all[0] = tok_ref[:, own_cols]

    for d in range(1, nz):
        tcopies[d - 1].wait_recv()
        remote(
            tok_all.at[d, mine], tok_all.at[d, mine], tf_send.at[d], tf_recv.at[d], ep, sib
        )
    wait_at = lambda dst, ssem, rsem: remote(dst, dst, ssem, rsem, ep, sib, go=False).wait_recv()

    def wait_on(ssem, rsem, dst):
        wait_at(dst, ssem, rsem)

    for i in range(2):
        remote(weights.at[i, x], weights.at[i, 1 - x], w_send.at[i], w_recv.at[i], pair, tp, go=False).wait_recv()
    for d in range(1, nz):
        wait_on(tf_send.at[d], tf_recv.at[d], tok_all.at[d, theirs])
    toks_in = tok_all[...].reshape(nz * toks, feat)
    fh = feat // 2
    sums = []
    for i in range(2):
        total = jnp.dot(toks_in[:, :fh], weights[i, 0], preferred_element_type=f32) + jnp.dot(
            toks_in[:, fh:], weights[i, 1], preferred_element_type=f32
        )
        sums.append(total[:toks])
        for d in range(1, nz):
            part_send[d - 1, i] = total[d * toks : (d + 1) * toks].astype(bf16)
    pcopies = []
    for d in range(1, nz):
        pcopies.append(
            remote(
                part_send.at[d - 1], part_recv.at[d - 1], p_send.at[d], p_recv.at[d], line(-d), tp
            )
        )

    for d in range(1, n):
        rcopies[d - 1].wait_recv()
        remote(
            rows_all.at[tp, d], rows_all.at[tp, d], rf_send.at[d], rf_recv.at[d], ep, sib
        )
        ecopies[d - 1].wait_recv()
        remote(
            ext_all.at[tp, d], ext_all.at[tp, d], rf_send.at[n + d], rf_recv.at[n + d], ep, sib
        )
    for load in loads[:2]:
        load.wait()
    for d in range(1, n):
        wait_on(rf_send.at[d], rf_recv.at[d], rows_all.at[sib, d])
        wait_on(rf_send.at[n + d], rf_recv.at[n + d], ext_all.at[sib, d])
    ext_wide[...] = ext_all[...].astype(f32)
    every = half_send.shape[0]

    def stacked(h):
        parts = [rows_all[h].astype(f32).reshape(n * base, halfw)]
        for k in range(extra):
            parts.append(
                jnp.concatenate([ext_wide[h, :, k * chunks + c, :] for c in range(chunks)], 1)
            )
        if every > n * slots:
            parts.append(jnp.zeros((every - n * slots, halfw), f32))
        return jnp.concatenate(parts, 0).astype(bf16)

    low, high = stacked(0), stacked(1)

    def project(w):
        return jnp.dot(low, w[:halfw], preferred_element_type=f32) + jnp.dot(
            high, w[halfw:], preferred_element_type=f32
        )

    gate = project(eg)
    up = project(eu)
    act = (gate / (1.0 + jnp.exp(-gate)) * up).astype(bf16)
    for d in range(1, nz):
        pcopies[d - 1].wait_recv()
        sums = [sums[i] + part_recv[d - 1, i].astype(f32) for i in range(2)]
    dense_hidden = (sums[0] / (1.0 + jnp.exp(-sums[0])) * sums[1]).astype(bf16)
    hid_all[0] = dense_hidden
    hcopies = []
    for d in range(1, nz):
        hcopies.append(
            remote(hid_all.at[0], hid_all.at[d], h_send.at[d], h_recv.at[d], line(d), tp)
        )

    loads[2].wait()
    off = pl.ds(pl.multiple_of(sib * halfw, halfw), halfw)
    keep = pl.ds(pl.multiple_of(tp * halfw, halfw), halfw)
    half_send[...] = jnp.dot(act, ed[:, off], preferred_element_type=f32).astype(bf16)
    scopy = remote(half_send, half_recv, s_send, s_recv, ep, sib)

    own_half = jnp.dot(act, ed[:, keep], preferred_element_type=f32).astype(bf16)
    scopy.wait_recv()
    member = own_half.astype(f32) + half_recv[...].astype(f32)
    ret_send[...] = member[: n * base].reshape(n, base, halfw).astype(bf16)
    for k in range(extra):
        first = n * (base + k)
        for c in range(chunks):
            ext_wide[0, :, k * chunks + c, :] = member[first : first + n, c * 128 : (c + 1) * 128]
    rex_send[...] = ext_wide[0].astype(bf16)
    mcopies, xcopies = [], []
    for d in range(1, n):
        mcopies.append(
            remote(ret_send.at[d], ret_recv.at[d - 1], m_send.at[d], m_recv.at[d], ring(-d), tp)
        )
        xcopies.append(
            remote(
                rex_send.at[d], rex_recv.at[d - 1], m_send.at[n + d], m_recv.at[n + d], ring(-d), tp
            )
        )

    remote(weights.at[2, x], weights.at[2, 1 - x], w_send.at[2], w_recv.at[2], pair, tp, go=False).wait_recv()
    for d in range(1, nz):
        hcopies[d - 1].wait_recv()
    owner = lax.div(z, pos_count)
    place = lax.rem(z, pos_count)
    hid_in = hid_all[...].reshape(nz * toks, hidden)
    away = jnp.dot(hid_in, weights[2, sib], preferred_element_type=f32)
    pre_send[...] = away.astype(bf16)
    qcopy = remote(pre_send, pre_recv, q_send, q_recv, ep, sib)
    part = jnp.dot(hid_in, weights[2, tp], preferred_element_type=f32)
    qcopy.wait_recv()
    part = part + pre_recv[...].astype(f32)
    down_send[...] = part.astype(bf16).reshape(nz, toks, fh)
    for d in range(1, nz):
        remote(
            down_send.at[d],
            down_recv.at[place, tp],
            d_send.at[d],
            d_recv.at[place, tp],
            line(-d),
            owner,
        )

    def sibling_copy():
        return remote(
            down_send.at[0],
            down_recv.at[place, tp],
            d_send.at[0],
            d_recv.at[place, tp],
            ep,
            sib,
            go=False,
        )

    @pl.when(owner != tp)
    def _():
        sibling_copy().start()

    @pl.when(owner == tp)
    def _():
        down_recv[place, tp] = down_send[0]

    total = ret_send[0].astype(f32)
    ext_total = rex_send[0].astype(f32)
    for d in range(1, n):
        mcopies[d - 1].wait_recv()
        xcopies[d - 1].wait_recv()
        total = total + ret_recv[d - 1].astype(f32)
        ext_total = ext_total + rex_recv[d - 1].astype(f32)
    if spad > base:
        row_id = lax.broadcasted_iota(jnp.int32, (spad - base, halfw), 0)
        tail = jnp.zeros((spad - base, halfw), f32)
        for k in range(extra):
            row = jnp.concatenate(
                [ext_total[k * chunks + c : k * chunks + c + 1, :] for c in range(chunks)], 1
            )
            tail = jnp.where(row_id == k, row, tail)
        total = jnp.concatenate([total, tail], 0)
    spread = jnp.where(match, table[8:9, :], 0.0)[:, :spad]
    combined = jnp.dot(
        spread, total, preferred_element_type=f32, precision=lax.Precision.HIGHEST
    )
    for p in range(pos_count):
        for t in range(2):

            @pl.when(jnp.logical_or(tp * pos_count + p != z, tp != t))
            def _():
                wait_on(d_send.at[0], d_recv.at[p, t], down_recv.at[p, t])

        for t in range(2):
            cols = slice(p * feat + t * fh, p * feat + (t + 1) * fh)
            dense = down_recv[p, t].astype(f32)
            scale = 1.0 / (1.0 + jnp.exp(-bg_ref[:, cols]))
            out_ref[:, cols] = (combined[:, cols] + scale * dense).astype(bf16)

    for copy in sends:
        copy.wait_send()

    @pl.when(owner != tp)
    def _():
        sibling_copy().wait_send()


def fused_local(n, *args):
    tokens, chosen, dense_gate, branch_gate = args[0], args[1], args[6], args[9]
    toks, width = tokens.shape
    nz = n // 2
    feat = width // nz
    slots = chosen.shape[2]
    base = slots // 8 * 8
    lines = (slots - base) * (width // 256)
    every = -(-n * slots // 16) * 16
    hid = dense_gate.shape[1]
    units = args[3].shape[1]
    bf16 = jnp.bfloat16
    vmem = pl.BlockSpec(memory_space=pltpu.VMEM)
    hbm = pl.BlockSpec(memory_space=pl.ANY)
    dma = pltpu.SemaphoreType.DMA
    scratch = [
        pltpu.VMEM((toks, width), bf16),
        pltpu.VMEM((width, units), bf16),
        pltpu.VMEM((width, units), bf16),
        pltpu.VMEM((units, width), bf16),
        pltpu.VMEM((3, 2) + dense_gate.shape, bf16),
        pltpu.VMEM((nz, toks, feat), bf16),
        pltpu.VMEM((16, 128), jnp.float32),
        pltpu.VMEM((2, n, base, width // 2), bf16),
        pltpu.VMEM((2, n, lines, 128), bf16),
        pltpu.VMEM((2, n, lines, 128), jnp.float32),
        pltpu.VMEM((nz - 1, 2, toks, hid), bf16),
        pltpu.VMEM((nz - 1, 2, toks, hid), bf16),
        pltpu.VMEM((nz, toks, hid), bf16),
        pltpu.VMEM((nz, toks, feat // 2), bf16),
        pltpu.VMEM((nz // 2, 2, toks, feat // 2), bf16),
        pltpu.VMEM((nz * toks, feat // 2), bf16),
        pltpu.VMEM((nz * toks, feat // 2), bf16),
        pltpu.VMEM((every, width // 2), bf16),
        pltpu.VMEM((every, width // 2), bf16),
        pltpu.VMEM((n, base, width // 2), bf16),
        pltpu.VMEM((n - 1, base, width // 2), bf16),
        pltpu.VMEM((n, lines, 128), bf16),
        pltpu.VMEM((n - 1, lines, 128), bf16),
        dma((7,)),
        dma((3,)),
        dma((3,)),
        dma((nz,)),
        dma((nz,)),
        dma((nz,)),
        dma((nz,)),
        dma((2 * n,)),
        dma((2 * n,)),
        dma((2 * n,)),
        dma((2 * n,)),
        dma((nz,)),
        dma((nz,)),
        dma((nz,)),
        dma((nz,)),
        dma((nz,)),
        dma((nz // 2, 2)),
        dma,
        dma,
        dma,
        dma,
        dma((2 * n,)),
        dma((2 * n,)),
    ]
    return pl.pallas_call(
        functools.partial(fused_kernel, n),
        out_shape=jax.ShapeDtypeStruct((toks, width // 2), bf16),
        in_specs=[hbm] + [vmem] * 2 + [hbm] * 6 + [vmem],
        out_specs=vmem,
        scratch_shapes=scratch,
        compiler_params=pltpu.CompilerParams(collective_id=0, has_side_effects=True),
    )(*args[:9], branch_gate.reshape(1, -1))


def local(*args):
    n = lax.axis_size("ep")
    tokens, chosen, dense_gate = args[0], args[1], args[6]
    width = tokens.shape[1]
    square = dense_gate.shape[0] == dense_gate.shape[1] == args[8].shape[1]
    fits = chosen.shape[0] == 1 and n % 4 == 0 and square
    fits = fits and (width // n) % 128 == 0 and tokens.shape[0] % 32 == 0
    fits = fits and chosen.shape[2] > 8 and chosen.shape[2] % 8 != 0 and width % 2048 == 0
    fits = fits and chosen.shape[2] <= 128 and lax.axis_size("tp") == 2
    return fused_local(n, *args) if fits else plain_local(*args)


def plain_local(
    tokens,
    chosen,
    route_weight,
    expert_gate,
    expert_up,
    expert_down,
    dense_gate,
    dense_up,
    dense_down,
    branch_gate,
):
    ep_count = lax.axis_size("ep")
    experts = chosen.shape[0]
    slots = chosen.shape[2]
    tok_local = tokens.shape[0]
    width = tokens.shape[1]
    picked = chosen[:, 0, :]
    filled = picked >= 0
    token_rows = jnp.take(tokens, jnp.maximum(picked, 0).reshape(-1), axis=0).reshape(
        experts, slots, width
    )
    token_rows = jnp.where(filled[:, :, None], token_rows, jnp.zeros((), jnp.bfloat16))
    send_width = token_rows.shape[2]
    piece = send_width // 8
    split_rows = jnp.transpose(token_rows.reshape(experts, slots, 8, piece), (0, 2, 1, 3)).reshape(
        ep_count, slots, piece
    )
    own_piece = lax.all_to_all(split_rows, "ep", split_axis=0, concat_axis=0, tiled=True)
    member = lax.axis_index("ep") % 8
    current = own_piece[:, :, None, :]
    partner = swapped(current, "ep", 0)
    current = join_pieces(current, partner, member % 2 == 1)
    partner = swapped(current, "ep", 1)
    current = join_pieces(current, partner, member // 2 % 2 == 1)
    partner = swapped(current, "ep", 2)
    current = join_pieces(current, partner, member // 4 == 1)
    received = current.reshape(ep_count, slots, send_width)
    hidden = expert_hidden(received, gate_cols=expert_gate, up_cols=expert_up)
    flat_hidden = hidden.reshape(ep_count * slots, -1)
    shard_rows = expert_down
    member_sums = lax.psum_scatter(
        lax.dot_general(
            shard_rows, flat_hidden, (((0,), (1,)), ((), ())), preferred_element_type=jnp.float32
        ).astype(jnp.bfloat16),
        "tp",
        scatter_dimension=0,
        tiled=True,
    )
    returned = lax.all_to_all(member_sums, "ep", split_axis=1, concat_axis=1, tiled=True)
    summed = returned.astype(jnp.float32).reshape(width // 2, experts, 8, slots).sum(axis=2)
    positions = lax.broadcasted_iota(jnp.int32, (experts, slots, tok_local), 2)
    weights_table = jnp.where(picked[:, :, None] == positions, route_weight[:, 0, :, None], 0.0)
    combined = jnp.einsum("fek,ekt->tf", summed, weights_table, precision=lax.Precision.HIGHEST)
    shard_rows = (
        lax.all_gather(dense_gate, "ep", axis=0, tiled=True),
        lax.all_gather(dense_up, "ep", axis=0, tiled=True),
    )
    gate_dense = jnp.dot(tokens, shard_rows[0], preferred_element_type=jnp.float32)
    up_dense = jnp.dot(tokens, shard_rows[1], preferred_element_type=jnp.float32)
    dense_hidden = (jax.nn.silu(gate_dense) * up_dense).astype(jnp.bfloat16)
    dense_terms = jnp.dot(
        dense_hidden,
        lax.all_gather(dense_down, "ep", axis=1, tiled=True),
        preferred_element_type=jnp.float32,
    )
    dense_sum = lax.psum_scatter(
        dense_terms.astype(jnp.bfloat16), "tp", scatter_dimension=1, tiled=True
    ).astype(jnp.float32)
    return (combined + jax.nn.sigmoid(branch_gate)[None, :] * dense_sum).astype(jnp.bfloat16)


def solution(mesh):
    return jax.shard_map(
        local,
        mesh=mesh,
        in_specs=(
            P(("grp", "ep"), None),
            P(None, ("grp", "ep"), None),
            P(None, ("grp", "ep"), None),
            P(None, ("ep", "tp")),
            P(None, ("ep", "tp")),
            P(("ep", "tp"), None),
            P("ep", "tp"),
            P("ep", "tp"),
            P("tp", "ep"),
            P("tp"),
        ),
        out_specs=P(("grp", "ep"), "tp"),
        check_vma=False,
    )
```
